32 devices in a mesh: sp: 8 (over z, core), tp: 4 (over y, x).
Axes of the slice: x: 2, y: 2, z: 4, core: 2. Of those that a mesh axis runs over, the one named last changes fastest.
Arguments:
- tokens: bfloat16 [6144, 2048], P('sp', 'tp'), may hold values from -26 to 26, as said below
- mix_gain: bfloat16 [2, 2048], replicated, may hold values from 0.099609375 to 1.8984375
- x_weight: bfloat16 [2, 2048, 1024], P(None, 'sp', 'tp'), may hold values from -0.125 to 0.125
- gate_weight: bfloat16 [2, 2048, 1024], P(None, 'sp', 'tp'), may hold values from -0.125 to 0.125
- conv_taps: bfloat16 [2, 4, 1024], P(None, None, 'tp'), may hold values from -3 to 3
- a_maps: bfloat16 [2, 16, 64, 64], P(None, 'tp'), may hold values from -0.75 to 0.75
- i_maps: bfloat16 [2, 16, 64, 64], P(None, 'tp'), may hold values from -0.75 to 0.75
- decay_rate: float32 [2, 1024], P(None, 'tp'), as said below
- pace: float32 [6144], P('sp'), may hold values from 0.35 to 2.8, as said below
- jumps: float32 [6144], P('sp'), may hold values from -0.7 to 0, as said below
- out_gain: bfloat16 [2, 1024], P(None, 'tp'), may hold values from 0.099609375 to 1.8984375
- out_weight: bfloat16 [2, 1024, 2048], P(None, 'sp', 'tp'), may hold values from -0.1875 to 0.1875
Outputs:
- stream: bfloat16 [6144, 2048], P('sp', 'tp')
The draws below stay inside these ranges and needn't reach their ends.
Inputs may be any that keep to these rules, and one draw needn't show every extreme that they name: `tokens`: random-looking real values; feature scales differ along the features. `decay_rate`: positive. `pace`: positive. `jumps`: zero or negative.
All inputs are finite; a program needn't handle non-finite values.
Results may differ from the reference program's by a relative error of at most 0.01.
Values may be sent and summed in bfloat16 or wider, within the bound.
A program may use at most 64 MiB of HBM per device.

```python
import math
import jax
import jax.numpy as jnp
from jax import lax

D = 2048
D_REC = 1024
HEAD = 64
WIDTH = 4
LAYERS = 2
TOK_DEV = 768
TOKENS = 6144
HEADS = 16


def draw_tokens(key, part):
    first = jax.random.fold_in(key, 11)
    second = jax.random.fold_in(key, 12)
    ramp = jnp.exp(jnp.linspace(0.0, math.log(3.0), D)).astype(jnp.float32)
    rough = jnp.exp(jax.random.uniform(second, (D,), jnp.float32, -0.35, 0.35))
    values = jnp.clip(jax.random.normal(first, (TOKENS, D), jnp.float32), -6.0, 6.0)
    return (values * ramp[None, :] * rough[None, :]).astype(jnp.bfloat16)


def draw_decay_rate(key, part):
    first = jax.random.fold_in(key, 21)
    second = jax.random.fold_in(key, 22)
    third = jax.random.fold_in(key, 23)
    share = 0.5
    fast = jax.random.uniform(first, (LAYERS, D_REC), jnp.float32) < share
    quick = jnp.exp(jax.random.uniform(second, (LAYERS, D_REC), jnp.float32, math.log(0.004), math.log(0.012)))
    slow = jnp.exp(jax.random.uniform(third, (LAYERS, D_REC), jnp.float32, math.log(0.02), math.log(0.1))) / TOKENS
    return jnp.where(fast, quick, slow).astype(jnp.float32)


def draw_pace(key, part):
    first = jax.random.fold_in(key, 31)
    second = jax.random.fold_in(key, 32)
    blocks = TOKENS // TOK_DEV
    block_factor = jnp.exp(jax.random.uniform(first, (blocks,), jnp.float32, math.log(0.5), math.log(2.0)))
    fine = jnp.exp(jax.random.uniform(second, (TOKENS,), jnp.float32, math.log(0.7), math.log(1.4)))
    return (jnp.repeat(block_factor, TOK_DEV) * fine).astype(jnp.float32)


def draw_jumps(key, part):
    first = jax.random.fold_in(key, 41)
    second = jax.random.fold_in(key, 42)
    spots = jax.random.randint(first, (6,), 0, TOKENS)
    sizes = jnp.log(jax.random.uniform(second, (6,), jnp.float32, 0.5, 0.8))
    return jnp.zeros((TOKENS,), jnp.float32).at[spots].set(sizes)


def levels(rng, shape, cuts, smallest, top_value):
    loudness = 1.0
    for position, parts in cuts:
        heights = jax.random.uniform(jax.random.fold_in(jax.random.fold_in(rng, 6), position), (parts,), jnp.float32, smallest / len(cuts), top_value / len(cuts))
        loudness = loudness * jnp.repeat(jnp.exp(heights), shape[position] // parts).reshape((-1,) + (1,) * (len(shape) - 1 - position))
    return loudness


def normal_values(stream_key, extent, deviation, limit, split=(), held_as=jnp.bfloat16):
    result = jax.random.normal(stream_key, extent, jnp.float32) * deviation
    if len(split) > 0:
        result = levels(stream_key, extent, split, -0.22, 0.18) * result
    return jnp.clip(result, min=-limit, max=limit).astype(held_as)


def setup_inputs(seed: int = 0) -> dict:
    seeds = jax.random.split(jax.random.key(seed), 13)
    return {
        "tokens": draw_tokens(jax.random.fold_in(seeds[12], 71), 0),
        "mix_gain": jnp.clip(1.0 + 0.18 * jax.random.normal(seeds[1], (LAYERS, D), jnp.float32), 0.099609375, 1.8984375).astype(jnp.bfloat16),
        "x_weight": normal_values(seeds[2], (LAYERS, D, D_REC), D ** -0.5, 0.125, ((1, 8), (2, 4))),
        "gate_weight": normal_values(seeds[3], (LAYERS, D, D_REC), D ** -0.5, 0.125, ((1, 8), (2, 4))),
        "conv_taps": normal_values(seeds[4], (LAYERS, WIDTH, D_REC), WIDTH ** -0.5, 3.0, ((2, 4),)),
        "a_maps": normal_values(seeds[5], (LAYERS, HEADS, HEAD, HEAD), HEAD ** -0.5, 0.75, ((1, 4),)),
        "i_maps": normal_values(seeds[6], (LAYERS, HEADS, HEAD, HEAD), HEAD ** -0.5, 0.75, ((1, 4),)),
        "decay_rate": draw_decay_rate(jax.random.fold_in(seeds[12], 71), 0),
        "pace": draw_pace(jax.random.fold_in(seeds[12], 71), 0),
        "jumps": draw_jumps(jax.random.fold_in(seeds[12], 71), 0),
        "out_gain": jnp.clip(1.0 + 0.18 * jax.random.normal(seeds[10], (LAYERS, D_REC), jnp.float32), 0.099609375, 1.8984375).astype(jnp.bfloat16),
        "out_weight": normal_values(seeds[11], (LAYERS, D_REC, D), D_REC ** -0.5, 0.1875, ((1, 8), (2, 4))),
    }


EPS = 1e-06
GATE_C = 8.0

def combine(first, second):
    return (first[0] * second[0], second[0] * first[1] + second[1])

def reference(tokens, mix_gain, x_weight, gate_weight, conv_taps, a_maps, i_maps, decay_rate, pace, jumps, out_gain, out_weight):
    f32 = jnp.float32
    stream = tokens
    for layer in range(LAYERS):
        xf = stream.astype(f32)
        normed = (xf * lax.rsqrt(lax.optimization_barrier(jnp.mean(xf * xf, axis=1, keepdims=True)) + EPS) * mix_gain[layer].astype(f32)).astype(jnp.bfloat16)
        xr = jnp.dot(normed, x_weight[layer], preferred_element_type=f32).astype(jnp.bfloat16)
        gr = jnp.dot(normed, gate_weight[layer], preferred_element_type=f32).astype(jnp.bfloat16)
        padded = jnp.pad(xr, ((WIDTH - 1, 0), (0, 0))).astype(f32)
        taps = conv_taps[layer].astype(f32)
        conv = jnp.zeros((TOKENS, D_REC), f32)
        for k in range(WIDTH):
            conv = conv + taps[k][None, :] * padded[k:k + TOKENS]
        xc = conv.astype(jnp.bfloat16)
        grouped = xc.astype(f32).reshape(TOKENS, HEADS, HEAD)
        rgate = jax.nn.sigmoid(jnp.einsum('thi,hij->thj', grouped, a_maps[layer].astype(f32)).reshape(TOKENS, D_REC))
        igate = jax.nn.sigmoid(jnp.einsum('thi,hij->thj', grouped, i_maps[layer].astype(f32)).reshape(TOKENS, D_REC))
        log_a = -GATE_C * rgate * decay_rate[layer][None, :] * pace[:, None] + jumps[:, None]
        decay = jnp.exp(log_a)
        drive = jnp.sqrt(-jnp.expm1(2.0 * log_a)) * igate * xc.astype(f32)
        _, state = lax.associative_scan(combine, (decay, drive), axis=0)
        rec = state * jax.nn.gelu(gr.astype(f32))
        scale = lax.rsqrt(lax.optimization_barrier(jnp.mean(rec * rec, axis=1, keepdims=True)) + EPS)
        mixed = (rec * out_gain[layer].astype(f32)[None, :]).astype(jnp.bfloat16)
        stream = (xf + jnp.dot(mixed, out_weight[layer], preferred_element_type=f32) * scale).astype(jnp.bfloat16)
    return stream
```

```python
import functools

import jax
import jax.numpy as jnp
from jax import lax
from jax.experimental import pallas as pl
from jax.experimental.pallas import tpu as pltpu
from jax.sharding import PartitionSpec as P

EPS = 1e-06
GATE_C = 8.0
WIDTH = 4
PAD = 8
SEGS = 8
F32 = jnp.float32
BF16 = jnp.bfloat16


def one_minus_exp(y):
    p = 1.0 / 5040.0
    for d in (720.0, 120.0, 24.0, 6.0, 2.0, 1.0):
        p = p * y + 1.0 / d
    return jnp.where(y > -0.35, -y * p, 1.0 - jnp.exp(y))


def kernel(
    dims,
    tokens, gain, xw, gw, taps, am, im, rate, pj, og, ow,
    out,
    xs, mx, wx, wg, wo, bda, bdi, xp, gl, a_s, b_s, ea_s, eb_s, tot, st, ogf,
    sem_send, sem_recv, w_send, w_fsend, w_recv, w_part, own_sem, tok_sem,
    rim_sem, st_send, st_recv, og_send, og_recv,
):
    n_sp, n_tp, layers, chunks = dims
    me = lax.axis_index("sp")
    my = lax.axis_index("tp")
    tok_rows, cols = tokens.shape
    ch = xw.shape[2]
    t_rows = tok_rows // chunks
    seg = t_rows // SEGS
    relay = n_tp == 4
    n_z = n_sp // 2
    z, k = me // 2, me % 2
    partner = 2 * z + 1 - k

    def dev(sp=None, tp=None):
        return {"sp": me if sp is None else sp, "tp": my if tp is None else tp}

    barrier = pltpu.get_barrier_semaphore()
    for d in range(1, n_sp):
        pl.semaphore_signal(barrier, inc=1, device_id=dev(sp=(me + d) % n_sp))
    for d in range(1, n_tp):
        pl.semaphore_signal(barrier, inc=1, device_id=dev(tp=(my + d) % n_tp))
    pl.semaphore_wait(barrier, n_sp + n_tp - 2)

    if relay:
        xb, yb = my % 2, my // 2
        xn = yb * 2 + (1 - xb)
        yn = (1 - yb) * 2 + xb
        direct = [(0, xn), (1, yn)]
        senders = [xn, yn]
        far = 3 - my
    else:
        direct = [(d, (my + d) % n_tp) for d in range(1, n_tp)]
        senders = [(my + d) % n_tp for d in range(1, n_tp)]
        far = None
    bufs = (xs, mx)

    def rows(c):
        return pl.ds(pl.multiple_of(c * t_rows, t_rows), t_rows)

    def own_copies(kind, l, c):
        buf = bufs[kind]
        place = buf.at[l, my, rows(c)]
        src = tokens.at[rows(c)] if (kind == 0 and l == 0) else place
        return [
            pltpu.make_async_remote_copy(
                src_ref=src, dst_ref=place,
                send_sem=sem_send.at[kind, l, c, slot], recv_sem=sem_recv.at[kind, l, c, my],
                device_id=dev(tp=peer),
            )
            for slot, peer in direct
        ]

    def send_own(kind, l, c):
        for copy in own_copies(kind, l, c):
            copy.start()

    def arrived(kind, l, c, src):
        place = bufs[kind].at[l, src, rows(c)]
        pltpu.make_async_copy(place, place, sem_recv.at[kind, l, c, src]).wait()

    def fwd_copy(kind, l, c):
        par = c % 2
        src = xn * (1 - par) + yn * par
        dst = yn * (1 - par) + xn * par
        place = bufs[kind].at[l, src, rows(c)]
        return pltpu.make_async_remote_copy(
            src_ref=place, dst_ref=place,
            send_sem=sem_send.at[kind, l, c, 2], recv_sem=sem_recv.at[kind, l, c, src],
            device_id=dev(tp=dst),
        )

    def near(kind, l, c):
        for s in senders:
            arrived(kind, l, c, s)
        if relay:
            fwd_copy(kind, l, c).start()

    def farther(kind, l, c):
        if relay:
            arrived(kind, l, c, far)

    w_args = (xw, gw, ow)
    w_bufs = (wx, wg, wo)

    def w_block(i, l, who):
        blk = w_args[i].shape[1]
        return w_bufs[i].at[l, pl.ds(pl.multiple_of(who * blk, blk), blk)]

    def w_copies(i, l):
        place = w_block(i, l, me)
        res = [
            pltpu.make_async_remote_copy(
                src_ref=w_args[i].at[l], dst_ref=place,
                send_sem=w_send.at[i, l], recv_sem=w_recv.at[i, l],
                device_id=dev(sp=((z + d) % n_z) * 2 + k),
            )
            for d in range(1, n_z)
        ]
        res.append(
            pltpu.make_async_remote_copy(
                src_ref=w_args[i].at[l], dst_ref=place,
                send_sem=w_send.at[i, l], recv_sem=w_part.at[i, l],
                device_id=dev(sp=partner),
            )
        )
        return res

    def w_own(i, l):
        return pltpu.make_async_copy(w_args[i].at[l], w_block(i, l, me), own_sem.at[i, l])

    def w_wait(i, l, sem, count):
        blk = w_args[i].shape[1]
        part = w_bufs[i].at[l, pl.ds(0, count * blk)]
        pltpu.make_async_copy(part, part, sem).wait()

    def w_forward(i, l):
        w_wait(i, l, w_recv.at[i, l], n_z - 1)
        for d in range(1, n_z):
            who = ((z + d) % n_z) * 2 + k
            pltpu.make_async_remote_copy(
                src_ref=w_block(i, l, who), dst_ref=w_block(i, l, who),
                send_sem=w_fsend.at[i, l], recv_sem=w_part.at[i, l],
                device_id=dev(sp=partner),
            ).start()

    def w_ready(i, l):
        w_wait(i, l, w_part.at[i, l], n_z)
        w_own(i, l).wait()

    tok_copy = pltpu.make_async_copy(tokens, xs.at[0, my], tok_sem)
    for c in range(chunks - 1, max(chunks - 3, -1), -1):
        send_own(0, 0, c)
    tok_copy.start()
    for l in range(layers):
        for i in range(3):
            for copy in w_copies(i, l):
                copy.start()
            w_own(i, l).start()

    row8 = lax.broadcasted_iota(jnp.int32, (8, ch), 0)
    ogv = og[...].astype(F32)
    acc = jnp.zeros((8, ch), F32)
    for l in range(layers):
        acc = jnp.where(row8 == l, ogv[l : l + 1], acc)
    ogf[my] = acc
    og_copies = [
        pltpu.make_async_remote_copy(
            src_ref=ogf.at[my], dst_ref=ogf.at[my],
            send_sem=og_send.at[d], recv_sem=og_recv.at[my],
            device_id=dev(tp=(my + d) % n_tp),
        )
        for d in range(1, n_tp)
    ]
    for copy in og_copies:
        copy.start()
    heads, head = am.shape[1], am.shape[2]
    for l in range(layers):
        for src, dst in ((am, bda), (im, bdi)):
            for h in range(heads):
                m = src[l, h].astype(F32)
                parts = [m if j == h else jnp.zeros((head, head), F32) for j in range(heads)]
                line = jnp.concatenate(parts, axis=1) if heads > 1 else m
                dst[l, h * head : (h + 1) * head, :] = line.astype(BF16)
    for l in range(layers):
        @pl.when(me == 0)
        def _():
            xp[l, 0:PAD, :] = jnp.zeros((PAD, ch), F32)

    def rim_copy(l):
        return pltpu.make_async_remote_copy(
            src_ref=xp.at[l, pl.ds(tok_rows, PAD)], dst_ref=xp.at[l, pl.ds(0, PAD)],
            send_sem=rim_sem.at[l, 0], recv_sem=rim_sem.at[l, 1],
            device_id=dev(sp=(me + 1) % n_sp),
        )

    def project(l, c):
        r = rows(c)
        total = jnp.zeros((t_rows, 1), F32)
        for p in range(n_tp):
            v = xs[l, p, r, :].astype(F32)
            total = total + jnp.sum(v * v, axis=1, keepdims=True)
        rs = lax.rsqrt(total / (n_tp * cols) + EPS)
        xr = jnp.zeros((t_rows, ch), F32)
        gr = jnp.zeros((t_rows, ch), F32)
        for p in range(n_tp):
            v = xs[l, p, r, :].astype(F32)
            g = gain[l : l + 1, p * cols : (p + 1) * cols].astype(F32)
            nv = (v * rs * g).astype(BF16)
            xr += jnp.dot(nv, wx[l, p * cols : (p + 1) * cols, :], preferred_element_type=F32)
            gr += jnp.dot(nv, wg[l, p * cols : (p + 1) * cols, :], preferred_element_type=F32)
        xp[l, pl.ds(pl.multiple_of(c * t_rows + PAD, 8), t_rows), :] = xr.astype(BF16).astype(F32)
        gl[c] = jax.nn.gelu(gr.astype(BF16).astype(F32))

    def gates(l, c):
        blk = xp[l, pl.ds(pl.multiple_of(c * t_rows, 8), t_rows + PAD), :]
        conv = jnp.zeros((t_rows, ch), F32)
        for j in range(WIDTH):
            o = PAD - (WIDTH - 1) + j
            conv = conv + taps[l, j : j + 1, :].astype(F32) * blk[o : o + t_rows]
        xc = conv.astype(BF16)
        rg = jax.nn.sigmoid(jnp.dot(xc, bda[l], preferred_element_type=F32))
        ig = jax.nn.sigmoid(jnp.dot(xc, bdi[l], preferred_element_type=F32))
        pv = pj[rows(c), :]
        log_a = (-GATE_C * rate[l : l + 1, :]) * rg * pv[:, 0:1] + pv[:, 1:2]
        av = jnp.exp(log_a)
        bv = jnp.sqrt(one_minus_exp(2.0 * log_a)) * ig * xc.astype(F32)
        lw = a_s.shape[3]
        for q in range(a_s.shape[1]):
            a_s[c, q] = av[:, q * lw : (q + 1) * lw]
            b_s[c, q] = bv[:, q * lw : (q + 1) * lw]
            pa = jnp.ones((SEGS, lw), F32)
            hb = jnp.zeros((SEGS, lw), F32)
            for j in range(seg):
                at = pl.ds(j, SEGS, stride=seg)
                x = a_s[c, q, at, :]
                hb = x * hb + b_s[c, q, at, :]
                pa = x * pa
                a_s[c, q, at, :] = pa
                b_s[c, q, at, :] = hb
            ea = jnp.ones((1, lw), F32)
            eb = jnp.zeros((1, lw), F32)
            for s in range(SEGS):
                ea_s[c, q, s : s + 1, :] = ea
                eb_s[c, q, s : s + 1, :] = eb
                eb = pa[s : s + 1] * eb + hb[s : s + 1]
                ea = pa[s : s + 1] * ea
            tot[c, 0:1, q * lw : (q + 1) * lw] = ea
            tot[c, 1:2, q * lw : (q + 1) * lw] = eb

    def st_copy(l, to):
        return pltpu.make_async_remote_copy(
            src_ref=st.at[l, me], dst_ref=st.at[l, me],
            send_sem=st_send.at[l, to], recv_sem=st_recv.at[l, me],
            device_id=dev(sp=to),
        )

    def mix(l, c, inc):
        lw = a_s.shape[3]
        halves = []
        for q in range(a_s.shape[1]):
            part = inc[:, q * lw : (q + 1) * lw]
            lines = []
            for s in range(SEGS):
                entry = eb_s[c, q, s : s + 1, :] + ea_s[c, q, s : s + 1, :] * part
                at = slice(s * seg, (s + 1) * seg)
                lines.append(b_s[c, q, at, :] + a_s[c, q, at, :] * entry)
            halves.append(jnp.concatenate(lines, axis=0))
        state = jnp.concatenate(halves, axis=1) if len(halves) > 1 else halves[0]
        rec = state * gl[c]
        mx[l, my, rows(c), :] = (rec * og[l : l + 1, :].astype(F32)).astype(BF16)

    def update(l, c):
        r = rows(c)
        total = jnp.zeros((t_rows, 1), F32)
        acc = jnp.zeros((t_rows, cols), F32)
        for p in range(n_tp):
            m = mx[l, p, r, :]
            v = m.astype(F32) * (1.0 / ogf[p, l : l + 1, :])
            total = total + jnp.sum(v * v, axis=1, keepdims=True)
            acc += jnp.dot(m, wo[l, p * ch : (p + 1) * ch, :], preferred_element_type=F32)
        scale = lax.rsqrt(total / (n_tp * ch) + EPS)
        new = (xs[l, my, r, :].astype(F32) + acc * scale).astype(BF16)
        if l == layers - 1:
            out[r, :] = new
        else:
            xs[l + 1, my, r, :] = new
            send_own(0, l + 1, c)

    tok_copy.wait()
    for l in range(layers):
        def front(i, carry):
            c = chunks - 1 - i

            @pl.when(i < chunks)
            def _():
                near(0, l, c)
                if l == 0:
                    @pl.when(c >= 2)
                    def _():
                        send_own(0, 0, c - 2)

            @pl.when(i == 1)
            def _():
                w_forward(0, l)
                w_forward(1, l)
                w_ready(0, l)
                w_ready(1, l)

            @pl.when(i >= 1)
            def _():
                farther(0, l, c + 1)
                project(l, c + 1)

            @pl.when((i == 1) & (me < n_sp - 1))
            def _():
                rim_copy(l).start()

            @pl.when(i >= 2)
            def _():
                gates(l, c + 2)

            return carry

        lax.fori_loop(0, chunks + 1, front, 0)

        @pl.when(me > 0)
        def _():
            rim_copy(l).wait_recv()

        gates(l, 0)

        ta, tb = jnp.ones((1, ch), F32), jnp.zeros((1, ch), F32)
        for c in range(chunks):
            tb = tot[c, 0:1, :] * tb + tot[c, 1:2, :]
            ta = tot[c, 0:1, :] * ta
        st[l, me] = jnp.where(row8 == 0, ta, tb)

        def send_st(to, carry):
            st_copy(l, to).start()
            return carry

        lax.fori_loop(me + 1, n_sp, send_st, 0)
        w_forward(2, l)

        def take_st(src, inc):
            place = st.at[l, src]
            pltpu.make_async_copy(place, place, st_recv.at[l, src]).wait()
            return st[l, src, 0:1, :] * inc + st[l, src, 1:2, :]

        inc = lax.fori_loop(0, me, take_st, jnp.zeros((1, ch), F32))
        incs = []
        for c in range(chunks):
            incs.append(inc)
            inc = tot[c, 0:1, :] * inc + tot[c, 1:2, :]
        for c in range(chunks - 1, -1, -1):
            mix(l, c, incs[c])
            if c >= chunks - 2:
                send_own(1, l, c)
        w_ready(2, l)
        if l == 0:
            for d in range(1, n_tp):
                src = (my + d) % n_tp
                pltpu.make_async_copy(ogf.at[src], ogf.at[src], og_recv.at[src]).wait()

        def back(i, carry):
            c = chunks - 1 - i

            @pl.when(i < chunks)
            def _():
                near(1, l, c)

                @pl.when(c >= 2)
                def _():
                    send_own(1, l, c - 2)

            @pl.when(i >= 1)
            def _():
                farther(1, l, c + 1)
                update(l, c + 1)

            return carry

        lax.fori_loop(0, chunks + 1, back, 0)

    def drain(c, carry):
        for kind in range(2):
            for l in range(layers):
                for copy in own_copies(kind, l, c):
                    copy.wait_send()
                if relay:
                    fwd_copy(kind, l, c).wait_send()
        return carry

    lax.fori_loop(0, chunks, drain, 0)
    for l in range(layers):
        for i in range(3):
            w_wait(i, l, w_send.at[i, l], n_z)
            w_wait(i, l, w_fsend.at[i, l], n_z - 1)

        @pl.when(me < n_sp - 1)
        def _():
            rim_copy(l).wait_send()

        def st_done(to, carry):
            st_copy(l, to).wait_send()
            return carry

        lax.fori_loop(me + 1, n_sp, st_done, 0)
    for copy in og_copies:
        copy.wait_send()


def body(n_sp, n_tp, tokens, mix_gain, x_weight, gate_weight, conv_taps, a_maps, i_maps,
         decay_rate, pace, jumps, out_gain, out_weight):
    layers = x_weight.shape[0]
    tok_rows, cols = tokens.shape
    ch = x_weight.shape[2]
    d = n_tp * cols
    d_rec = n_tp * ch
    chunks = 4
    t_rows = tok_rows // chunks
    lw = min(ch, 128)
    nq = ch // lw
    pj = jnp.stack([pace, jumps], axis=1)
    vm = pl.BlockSpec(memory_space=pltpu.VMEM)
    hb = pl.BlockSpec(memory_space=pl.ANY)
    dma = pltpu.SemaphoreType.DMA
    return pl.pallas_call(
        functools.partial(kernel, (n_sp, n_tp, layers, chunks)),
        out_shape=jax.ShapeDtypeStruct((tok_rows, cols), BF16),
        in_specs=[hb, vm, hb, hb, vm, vm, vm, vm, vm, vm, hb],
        out_specs=vm,
        scratch_shapes=[
            pltpu.VMEM((layers, n_tp, tok_rows, cols), BF16),
            pltpu.VMEM((layers, n_tp, tok_rows, ch), BF16),
            pltpu.VMEM((layers, d, ch), BF16),
            pltpu.VMEM((layers, d, ch), BF16),
            pltpu.VMEM((layers, d_rec, cols), BF16),
            pltpu.VMEM((layers, ch, ch), BF16),
            pltpu.VMEM((layers, ch, ch), BF16),
            pltpu.VMEM((layers, PAD + tok_rows, ch), F32),
            pltpu.VMEM((chunks, t_rows, ch), F32),
            pltpu.VMEM((chunks, nq, t_rows, lw), F32),
            pltpu.VMEM((chunks, nq, t_rows, lw), F32),
            pltpu.VMEM((chunks, nq, SEGS, lw), F32),
            pltpu.VMEM((chunks, nq, SEGS, lw), F32),
            pltpu.VMEM((chunks, 8, ch), F32),
            pltpu.VMEM((layers, n_sp, 8, ch), F32),
            pltpu.VMEM((n_tp, 8, ch), F32),
            dma((2, layers, chunks, n_tp)),
            dma((2, layers, chunks, n_tp)),
            dma((3, layers)),
            dma((3, layers)),
            dma((3, layers)),
            dma((3, layers)),
            dma((3, layers)),
            dma,
            dma((layers, 2)),
            dma((layers, n_sp)),
            dma((layers, n_sp)),
            dma((n_tp,)),
            dma((n_tp,)),
        ],
        compiler_params=pltpu.CompilerParams(
            collective_id=0, has_side_effects=True, vmem_limit_bytes=60 * 1024 * 1024
        ),
    )(tokens, mix_gain, x_weight, gate_weight, conv_taps, a_maps, i_maps, decay_rate, pj,
      out_gain, out_weight)


def solution(mesh):
    in_specs = (
        P("sp", "tp"),
        P(),
        P(None, "sp", "tp"),
        P(None, "sp", "tp"),
        P(None, None, "tp"),
        P(None, "tp", None, None),
        P(None, "tp", None, None),
        P(None, "tp"),
        P("sp"),
        P("sp"),
        P(None, "tp"),
        P(None, "sp", "tp"),
    )
    out_specs = P("sp", "tp")
    return jax.shard_map(
        functools.partial(body, mesh.shape["sp"], mesh.shape["tp"]),
        mesh=mesh, in_specs=in_specs, out_specs=out_specs, check_vma=False,
    )
```

```python
import functools

import jax
import jax.numpy as jnp
from jax import lax
from jax.experimental import pallas as pl
from jax.experimental.pallas import tpu as pltpu
from jax.sharding import PartitionSpec as P

EPS = 1e-06
GATE_C = 8.0
WIDTH = 4
PAD = 8
SEGS = 8
F32 = jnp.float32
BF16 = jnp.bfloat16


def one_minus_exp(y):
    p = 1.0 / 5040.0
    for d in (720.0, 120.0, 24.0, 6.0, 2.0, 1.0):
        p = p * y + 1.0 / d
    return jnp.where(y > -0.35, -y * p, 1.0 - jnp.exp(y))


def kernel(
    dims,
    tokens, gain, xw, gw, taps, am, im, rate, pj, og, ow,
    out,
    xs, mx, wx, wg, wo, bda, bdi, xp, gl, a_s, b_s, ea_s, eb_s, tot, st, ogf,
    sem_send, sem_recv, w_send, w_fsend, w_recv, w_part, own_sem, tok_sem,
    rim_sem, st_send, st_recv, og_send, og_recv,
):
    n_sp, n_tp, layers, chunks = dims
    me = lax.axis_index("sp")
    my = lax.axis_index("tp")
    tok_rows, cols = tokens.shape
    ch = xw.shape[2]
    t_rows = tok_rows // chunks
    seg = t_rows // SEGS
    relay = n_tp == 4
    n_z = n_sp // 2
    z, k = me // 2, me % 2
    partner = 2 * z + 1 - k

    def dev(sp=None, tp=None):
        return {"sp": me if sp is None else sp, "tp": my if tp is None else tp}

    barrier = pltpu.get_barrier_semaphore()
    for d in range(1, n_sp):
        pl.semaphore_signal(barrier, inc=1, device_id=dev(sp=(me + d) % n_sp))
    for d in range(1, n_tp):
        pl.semaphore_signal(barrier, inc=1, device_id=dev(tp=(my + d) % n_tp))
    pl.semaphore_wait(barrier, n_sp + n_tp - 2)

    if relay:
        xb, yb = my % 2, my // 2
        xn = yb * 2 + (1 - xb)
        yn = (1 - yb) * 2 + xb
        direct = [(0, xn), (1, yn)]
        senders = [xn, yn]
        far = 3 - my
    else:
        direct = [(d, (my + d) % n_tp) for d in range(1, n_tp)]
        senders = [(my + d) % n_tp for d in range(1, n_tp)]
        far = None
    bufs = (xs, mx)

    def rows(c):
        return pl.ds(pl.multiple_of(c * t_rows, t_rows), t_rows)

    def own_copies(kind, l, c):
        buf = bufs[kind]
        place = buf.at[l, my, rows(c)]
        src = tokens.at[rows(c)] if (kind == 0 and l == 0) else place
        return [
            pltpu.make_async_remote_copy(
                src_ref=src, dst_ref=place,
                send_sem=sem_send.at[kind, l, c, slot], recv_sem=sem_recv.at[kind, l, c, my],
                device_id=dev(tp=peer),
            )
            for slot, peer in direct
        ]

    def send_own(kind, l, c):
        for copy in own_copies(kind, l, c):
            copy.start()

    def arrived(kind, l, c, src):
        place = bufs[kind].at[l, src, rows(c)]
        pltpu.make_async_copy(place, place, sem_recv.at[kind, l, c, src]).wait()

    def fwd_copies(kind, l, c):
        half = t_rows // 2
        res = []
        for n, (src, dst) in enumerate(((xn, yn), (yn, xn))):
            at = pl.ds(pl.multiple_of(c * t_rows + n * half, half), half)
            place = bufs[kind].at[l, src, at]
            res.append(
                pltpu.make_async_remote_copy(
                    src_ref=place, dst_ref=place,
                    send_sem=sem_send.at[kind, l, c, 2 + n], recv_sem=sem_recv.at[kind, l, c, src],
                    device_id=dev(tp=dst),
                )
            )
        return res

    def near(kind, l, c):
        for s in senders:
            arrived(kind, l, c, s)
        if relay:
            for copy in fwd_copies(kind, l, c):
                copy.start()

    def farther(kind, l, c):
        if relay:
            arrived(kind, l, c, far)

    w_args = (xw, gw, ow)
    w_bufs = (wx, wg, wo)

    def w_block(i, l, who):
        blk = w_args[i].shape[1]
        return w_bufs[i].at[l, pl.ds(pl.multiple_of(who * blk, blk), blk)]

    def w_copies(i, l):
        place = w_block(i, l, me)
        res = [
            pltpu.make_async_remote_copy(
                src_ref=w_args[i].at[l], dst_ref=place,
                send_sem=w_send.at[i, l], recv_sem=w_recv.at[i, l],
                device_id=dev(sp=((z + d) % n_z) * 2 + k),
            )
            for d in range(1, n_z)
        ]
        res.append(
            pltpu.make_async_remote_copy(
                src_ref=w_args[i].at[l], dst_ref=place,
                send_sem=w_send.at[i, l], recv_sem=w_part.at[i, l],
                device_id=dev(sp=partner),
            )
        )
        return res

    def w_issue(i, l):
        for copy in w_copies(i, l):
            copy.start()

    def w_own(i, l):
        return pltpu.make_async_copy(w_args[i].at[l], w_block(i, l, me), own_sem.at[i, l])

    def w_wait(i, l, sem, count):
        blk = w_args[i].shape[1]
        part = w_bufs[i].at[l, pl.ds(0, count * blk)]
        pltpu.make_async_copy(part, part, sem).wait()

    def w_forward(i, l):
        w_wait(i, l, w_recv.at[i, l], n_z - 1)
        for d in range(1, n_z):
            who = ((z + d) % n_z) * 2 + k
            pltpu.make_async_remote_copy(
                src_ref=w_block(i, l, who), dst_ref=w_block(i, l, who),
                send_sem=w_fsend.at[i, l], recv_sem=w_part.at[i, l],
                device_id=dev(sp=partner),
            ).start()

    def w_ready(i, l):
        w_wait(i, l, w_part.at[i, l], n_z)
        w_own(i, l).wait()

    tok_copy = pltpu.make_async_copy(tokens, xs.at[0, my], tok_sem)
    for c in range(chunks - 1, max(chunks - 3, -1), -1):
        send_own(0, 0, c)
    tok_copy.start()
    w_issue(0, 0)
    w_issue(1, 0)
    for l in range(layers):
        for i in range(3):
            w_own(i, l).start()

    row8 = lax.broadcasted_iota(jnp.int32, (8, ch), 0)
    ogv = og[...].astype(F32)
    acc = jnp.zeros((8, ch), F32)
    for l in range(layers):
        acc = jnp.where(row8 == l, ogv[l : l + 1], acc)
    ogf[my] = acc
    og_copies = [
        pltpu.make_async_remote_copy(
            src_ref=ogf.at[my], dst_ref=ogf.at[my],
            send_sem=og_send.at[d], recv_sem=og_recv.at[my],
            device_id=dev(tp=(my + d) % n_tp),
        )
        for d in range(1, n_tp)
    ]
    for copy in og_copies:
        copy.start()
    heads, head = am.shape[1], am.shape[2]
    for l in range(layers):
        for src, dst in ((am, bda), (im, bdi)):
            for h in range(heads):
                m = src[l, h].astype(F32)
                parts = [m if j == h else jnp.zeros((head, head), F32) for j in range(heads)]
                line = jnp.concatenate(parts, axis=1) if heads > 1 else m
                dst[l, h * head : (h + 1) * head, :] = line.astype(BF16)
    for l in range(layers):
        @pl.when(me == 0)
        def _():
            xp[l, 0:PAD, :] = jnp.zeros((PAD, ch), F32)

    def rim_copy(l):
        return pltpu.make_async_remote_copy(
            src_ref=xp.at[l, pl.ds(tok_rows, PAD)], dst_ref=xp.at[l, pl.ds(0, PAD)],
            send_sem=rim_sem.at[l, 0], recv_sem=rim_sem.at[l, 1],
            device_id=dev(sp=(me + 1) % n_sp),
        )

    def project(l, c):
        r = rows(c)
        total = jnp.zeros((t_rows, 1), F32)
        for p in range(n_tp):
            v = xs[l, p, r, :].astype(F32)
            total = total + jnp.sum(v * v, axis=1, keepdims=True)
        rs = lax.rsqrt(total / (n_tp * cols) + EPS)
        xr = jnp.zeros((t_rows, ch), F32)
        gr = jnp.zeros((t_rows, ch), F32)
        for p in range(n_tp):
            v = xs[l, p, r, :].astype(F32)
            g = gain[l : l + 1, p * cols : (p + 1) * cols].astype(F32)
            nv = (v * rs * g).astype(BF16)
            xr += jnp.dot(nv, wx[l, p * cols : (p + 1) * cols, :], preferred_element_type=F32)
            gr += jnp.dot(nv, wg[l, p * cols : (p + 1) * cols, :], preferred_element_type=F32)
        xp[l, pl.ds(pl.multiple_of(c * t_rows + PAD, 8), t_rows), :] = xr.astype(BF16).astype(F32)
        gl[c] = jax.nn.gelu(gr.astype(BF16).astype(F32))

    def gates(l, c):
        blk = xp[l, pl.ds(pl.multiple_of(c * t_rows, 8), t_rows + PAD), :]
        conv = jnp.zeros((t_rows, ch), F32)
        for j in range(WIDTH):
            o = PAD - (WIDTH - 1) + j
            conv = conv + taps[l, j : j + 1, :].astype(F32) * blk[o : o + t_rows]
        xc = conv.astype(BF16)
        rg = jax.nn.sigmoid(jnp.dot(xc, bda[l], preferred_element_type=F32))
        ig = jax.nn.sigmoid(jnp.dot(xc, bdi[l], preferred_element_type=F32))
        pv = pj[rows(c), :]
        log_a = (-GATE_C * rate[l : l + 1, :]) * rg * pv[:, 0:1] + pv[:, 1:2]
        av = jnp.exp(log_a)
        bv = jnp.sqrt(one_minus_exp(2.0 * log_a)) * ig * xc.astype(F32)
        lw = a_s.shape[3]
        for q in range(a_s.shape[1]):
            a_s[c, q] = av[:, q * lw : (q + 1) * lw]
            b_s[c, q] = bv[:, q * lw : (q + 1) * lw]
            pa = jnp.ones((SEGS, lw), F32)
            hb = jnp.zeros((SEGS, lw), F32)
            for j in range(seg):
                at = pl.ds(j, SEGS, stride=seg)
                x = a_s[c, q, at, :]
                hb = x * hb + b_s[c, q, at, :]
                pa = x * pa
                a_s[c, q, at, :] = pa
                b_s[c, q, at, :] = hb
            ea = jnp.ones((1, lw), F32)
            eb = jnp.zeros((1, lw), F32)
            for s in range(SEGS):
                ea_s[c, q, s : s + 1, :] = ea
                eb_s[c, q, s : s + 1, :] = eb
                eb = pa[s : s + 1] * eb + hb[s : s + 1]
                ea = pa[s : s + 1] * ea
            tot[c, 0:1, q * lw : (q + 1) * lw] = ea
            tot[c, 1:2, q * lw : (q + 1) * lw] = eb

    def st_copy(l, to):
        return pltpu.make_async_remote_copy(
            src_ref=st.at[l, me], dst_ref=st.at[l, me],
            send_sem=st_send.at[l, to], recv_sem=st_recv.at[l, me],
            device_id=dev(sp=to),
        )

    def mix(l, c, inc):
        lw = a_s.shape[3]
        halves = []
        for q in range(a_s.shape[1]):
            part = inc[:, q * lw : (q + 1) * lw]
            lines = []
            for s in range(SEGS):
                entry = eb_s[c, q, s : s + 1, :] + ea_s[c, q, s : s + 1, :] * part
                at = slice(s * seg, (s + 1) * seg)
                lines.append(b_s[c, q, at, :] + a_s[c, q, at, :] * entry)
            halves.append(jnp.concatenate(lines, axis=0))
        state = jnp.concatenate(halves, axis=1) if len(halves) > 1 else halves[0]
        rec = state * gl[c]
        mx[l, my, rows(c), :] = (rec * og[l : l + 1, :].astype(F32)).astype(BF16)

    def update(l, c):
        r = rows(c)
        total = jnp.zeros((t_rows, 1), F32)
        acc = jnp.zeros((t_rows, cols), F32)
        for p in range(n_tp):
            m = mx[l, p, r, :]
            v = m.astype(F32) * (1.0 / ogf[p, l : l + 1, :])
            total = total + jnp.sum(v * v, axis=1, keepdims=True)
            acc += jnp.dot(m, wo[l, p * ch : (p + 1) * ch, :], preferred_element_type=F32)
        scale = lax.rsqrt(total / (n_tp * ch) + EPS)
        new = (xs[l, my, r, :].astype(F32) + acc * scale).astype(BF16)
        if l == layers - 1:
            out[r, :] = new
        else:
            xs[l + 1, my, r, :] = new
            send_own(0, l + 1, c)

    tok_copy.wait()
    for l in range(layers):
        def front(i, carry):
            c = chunks - 1 - i

            @pl.when(i < chunks)
            def _():
                near(0, l, c)
                if l == 0:
                    @pl.when(c >= 2)
                    def _():
                        send_own(0, 0, c - 2)

            @pl.when(i == 1)
            def _():
                w_forward(0, l)
                w_forward(1, l)
                w_issue(2, l)
                w_ready(0, l)
                w_ready(1, l)

            @pl.when(i >= 1)
            def _():
                farther(0, l, c + 1)
                project(l, c + 1)

            @pl.when((i == 1) & (me < n_sp - 1))
            def _():
                rim_copy(l).start()

            @pl.when(i >= 2)
            def _():
                gates(l, c + 2)

            return carry

        lax.fori_loop(0, chunks + 1, front, 0)

        @pl.when(me > 0)
        def _():
            rim_copy(l).wait_recv()

        gates(l, 0)

        ta, tb = jnp.ones((1, ch), F32), jnp.zeros((1, ch), F32)
        for c in range(chunks):
            tb = tot[c, 0:1, :] * tb + tot[c, 1:2, :]
            ta = tot[c, 0:1, :] * ta
        st[l, me] = jnp.where(row8 == 0, ta, tb)

        def send_st(to, carry):
            st_copy(l, to).start()
            return carry

        lax.fori_loop(me + 1, n_sp, send_st, 0)
        w_forward(2, l)
        if l + 1 < layers:
            w_issue(0, l + 1)
            w_issue(1, l + 1)

        def take_st(src, inc):
            place = st.at[l, src]
            pltpu.make_async_copy(place, place, st_recv.at[l, src]).wait()
            return st[l, src, 0:1, :] * inc + st[l, src, 1:2, :]

        inc = lax.fori_loop(0, me, take_st, jnp.zeros((1, ch), F32))
        incs = []
        for c in range(chunks):
            incs.append(inc)
            inc = tot[c, 0:1, :] * inc + tot[c, 1:2, :]
        for c in range(chunks - 1, -1, -1):
            mix(l, c, incs[c])
            if c >= chunks - 2:
                send_own(1, l, c)
        w_ready(2, l)
        if l == 0:
            for d in range(1, n_tp):
                src = (my + d) % n_tp
                pltpu.make_async_copy(ogf.at[src], ogf.at[src], og_recv.at[src]).wait()

        def back(i, carry):
            c = chunks - 1 - i

            @pl.when(i < chunks)
            def _():
                near(1, l, c)

                @pl.when(c >= 2)
                def _():
                    send_own(1, l, c - 2)

            @pl.when(i >= 1)
            def _():
                farther(1, l, c + 1)
                update(l, c + 1)

            return carry

        lax.fori_loop(0, chunks + 1, back, 0)

    def drain(c, carry):
        for kind in range(2):
            for l in range(layers):
                for copy in own_copies(kind, l, c):
                    copy.wait_send()
                if relay:
                    for copy in fwd_copies(kind, l, c):
                        copy.wait_send()
        return carry

    lax.fori_loop(0, chunks, drain, 0)
    for l in range(layers):
        for i in range(3):
            w_wait(i, l, w_send.at[i, l], n_z)
            w_wait(i, l, w_fsend.at[i, l], n_z - 1)

        @pl.when(me < n_sp - 1)
        def _():
            rim_copy(l).wait_send()

        def st_done(to, carry):
            st_copy(l, to).wait_send()
            return carry

        lax.fori_loop(me + 1, n_sp, st_done, 0)
    for copy in og_copies:
        copy.wait_send()


def body(n_sp, n_tp, tokens, mix_gain, x_weight, gate_weight, conv_taps, a_maps, i_maps,
         decay_rate, pace, jumps, out_gain, out_weight):
    layers = x_weight.shape[0]
    tok_rows, cols = tokens.shape
    ch = x_weight.shape[2]
    d = n_tp * cols
    d_rec = n_tp * ch
    chunks = 4
    t_rows = tok_rows // chunks
    lw = min(ch, 128)
    nq = ch // lw
    pj = jnp.stack([pace, jumps], axis=1)
    vm = pl.BlockSpec(memory_space=pltpu.VMEM)
    hb = pl.BlockSpec(memory_space=pl.ANY)
    dma = pltpu.SemaphoreType.DMA
    return pl.pallas_call(
        functools.partial(kernel, (n_sp, n_tp, layers, chunks)),
        out_shape=jax.ShapeDtypeStruct((tok_rows, cols), BF16),
        in_specs=[hb, vm, hb, hb, vm, vm, vm, vm, vm, vm, hb],
        out_specs=vm,
        scratch_shapes=[
            pltpu.VMEM((layers, n_tp, tok_rows, cols), BF16),
            pltpu.VMEM((layers, n_tp, tok_rows, ch), BF16),
            pltpu.VMEM((layers, d, ch), BF16),
            pltpu.VMEM((layers, d, ch), BF16),
            pltpu.VMEM((layers, d_rec, cols), BF16),
            pltpu.VMEM((layers, ch, ch), BF16),
            pltpu.VMEM((layers, ch, ch), BF16),
            pltpu.VMEM((layers, PAD + tok_rows, ch), F32),
            pltpu.VMEM((chunks, t_rows, ch), F32),
            pltpu.VMEM((chunks, nq, t_rows, lw), F32),
            pltpu.VMEM((chunks, nq, t_rows, lw), F32),
            pltpu.VMEM((chunks, nq, SEGS, lw), F32),
            pltpu.VMEM((chunks, nq, SEGS, lw), F32),
            pltpu.VMEM((chunks, 8, ch), F32),
            pltpu.VMEM((layers, n_sp, 8, ch), F32),
            pltpu.VMEM((n_tp, 8, ch), F32),
            dma((2, layers, chunks, n_tp)),
            dma((2, layers, chunks, n_tp)),
            dma((3, layers)),
            dma((3, layers)),
            dma((3, layers)),
            dma((3, layers)),
            dma((3, layers)),
            dma,
            dma((layers, 2)),
            dma((layers, n_sp)),
            dma((layers, n_sp)),
            dma((n_tp,)),
            dma((n_tp,)),
        ],
        compiler_params=pltpu.CompilerParams(
            collective_id=0, has_side_effects=True, vmem_limit_bytes=60 * 1024 * 1024
        ),
    )(tokens, mix_gain, x_weight, gate_weight, conv_taps, a_maps, i_maps, decay_rate, pj,
      out_gain, out_weight)


def solution(mesh):
    in_specs = (
        P("sp", "tp"),
        P(),
        P(None, "sp", "tp"),
        P(None, "sp", "tp"),
        P(None, None, "tp"),
        P(None, "tp", None, None),
        P(None, "tp", None, None),
        P(None, "tp"),
        P("sp"),
        P("sp"),
        P(None, "tp"),
        P(None, "sp", "tp"),
    )
    out_specs = P("sp", "tp")
    return jax.shard_map(
        functools.partial(body, mesh.shape["sp"], mesh.shape["tp"]),
        mesh=mesh, in_specs=in_specs, out_specs=out_specs, check_vma=False,
    )
```

```python
import functools

import jax
import jax.numpy as jnp
from jax import lax
from jax.experimental import pallas as pl
from jax.experimental.pallas import tpu as pltpu
from jax.sharding import PartitionSpec as P

EPS = 1e-06
GATE_C = 8.0
WIDTH = 4
PAD = 8
SEGS = 8
F32 = jnp.float32
BF16 = jnp.bfloat16


def one_minus_exp(y):
    p = 1.0 / 5040.0
    for d in (720.0, 120.0, 24.0, 6.0, 2.0, 1.0):
        p = p * y + 1.0 / d
    return jnp.where(y > -0.35, -y * p, 1.0 - jnp.exp(y))


def kernel(
    dims,
    tokens, gain, xw, gw, taps, am, im, rate, pj, og, ow,
    out,
    nrm, xs, mx, wx, wg, wo, bda, bdi, xp, gl, a_s, b_s, ea_s, eb_s, tot, st, ogf,
    sem_send, sem_recv, w_send, w_fsend, w_recv, w_part, own_sem, tok_sem,
    rim_sem, st_send, st_recv, og_send, og_recv,
):
    n_sp, n_tp, layers, chunks = dims
    me = lax.axis_index("sp")
    my = lax.axis_index("tp")
    tok_rows, cols = tokens.shape
    ch = xw.shape[2]
    t_rows = tok_rows // chunks
    seg = t_rows // SEGS
    relay = n_tp == 4
    n_z = n_sp // 2
    z, k = me // 2, me % 2
    partner = 2 * z + 1 - k

    def dev(sp=None, tp=None):
        return {"sp": me if sp is None else sp, "tp": my if tp is None else tp}

    barrier = pltpu.get_barrier_semaphore()
    for d in range(1, n_sp):
        pl.semaphore_signal(barrier, inc=1, device_id=dev(sp=(me + d) % n_sp))
    for d in range(1, n_tp):
        pl.semaphore_signal(barrier, inc=1, device_id=dev(tp=(my + d) % n_tp))
    pl.semaphore_wait(barrier, n_sp + n_tp - 2)

    if relay:
        xb, yb = my % 2, my // 2
        xn = yb * 2 + (1 - xb)
        yn = (1 - yb) * 2 + xb
        direct = [(0, xn), (1, yn)]
        senders = [xn, yn]
        far = 3 - my
    else:
        direct = [(d, (my + d) % n_tp) for d in range(1, n_tp)]
        senders = [(my + d) % n_tp for d in range(1, n_tp)]
        far = None
    bufs = (xs, mx)

    def rows(c):
        return pl.ds(pl.multiple_of(c * t_rows, t_rows), t_rows)

    def own_copies(kind, l, c):
        buf = bufs[kind]
        place = buf.at[l, my, rows(c)]
        src = tokens.at[rows(c)] if (kind == 0 and l == 0) else place
        return [
            pltpu.make_async_remote_copy(
                src_ref=src, dst_ref=place,
                send_sem=sem_send.at[kind, l, c, slot], recv_sem=sem_recv.at[kind, l, c, my],
                device_id=dev(tp=peer),
            )
            for slot, peer in direct
        ]

    def send_own(kind, l, c):
        for copy in own_copies(kind, l, c):
            copy.start()

    def arrived(kind, l, c, src):
        place = bufs[kind].at[l, src, rows(c)]
        pltpu.make_async_copy(place, place, sem_recv.at[kind, l, c, src]).wait()

    def fwd_copies(kind, l, c):
        half = t_rows // 2
        res = []
        for n, (src, dst) in enumerate(((xn, yn), (yn, xn))):
            at = pl.ds(pl.multiple_of(c * t_rows + n * half, half), half)
            place = bufs[kind].at[l, src, at]
            res.append(
                pltpu.make_async_remote_copy(
                    src_ref=place, dst_ref=place,
                    send_sem=sem_send.at[kind, l, c, 2 + n], recv_sem=sem_recv.at[kind, l, c, src],
                    device_id=dev(tp=dst),
                )
            )
        return res

    def near(kind, l, c):
        for s in senders:
            arrived(kind, l, c, s)
        if relay:
            for copy in fwd_copies(kind, l, c):
                copy.start()

    def farther(kind, l, c):
        if relay:
            arrived(kind, l, c, far)

    w_args = (xw, gw, ow)
    w_bufs = (wx, wg, wo)

    def w_block(i, l, who):
        blk = w_args[i].shape[1]
        return w_bufs[i].at[l, pl.ds(pl.multiple_of(who * blk, blk), blk)]

    def w_copies(i, l):
        place = w_block(i, l, me)
        res = [
            pltpu.make_async_remote_copy(
                src_ref=w_args[i].at[l], dst_ref=place,
                send_sem=w_send.at[i, l], recv_sem=w_recv.at[i, l],
                device_id=dev(sp=((z + d) % n_z) * 2 + k),
            )
            for d in sorted(range(1, n_z), key=lambda d: (abs(2 * d - n_z), -d))
        ]
        res.append(
            pltpu.make_async_remote_copy(
                src_ref=w_args[i].at[l], dst_ref=place,
                send_sem=w_send.at[i, l], recv_sem=w_part.at[i, l],
                device_id=dev(sp=partner),
            )
        )
        return res

    def w_issue(i, l):
        for copy in w_copies(i, l):
            copy.start()

    def w_own(i, l):
        return pltpu.make_async_copy(w_args[i].at[l], w_block(i, l, me), own_sem.at[i, l])

    def w_wait(i, l, sem, count):
        blk = w_args[i].shape[1]
        part = w_bufs[i].at[l, pl.ds(0, count * blk)]
        pltpu.make_async_copy(part, part, sem).wait()

    def w_forward(i, l):
        w_wait(i, l, w_recv.at[i, l], n_z - 1)
        for d in range(1, n_z):
            who = ((z + d) % n_z) * 2 + k
            pltpu.make_async_remote_copy(
                src_ref=w_block(i, l, who), dst_ref=w_block(i, l, who),
                send_sem=w_fsend.at[i, l], recv_sem=w_part.at[i, l],
                device_id=dev(sp=partner),
            ).start()

    def w_ready(i, l):
        w_wait(i, l, w_part.at[i, l], n_z)
        w_own(i, l).wait()

    tok_copy = pltpu.make_async_copy(tokens, xs.at[0, my], tok_sem)
    for c in range(chunks - 1, max(chunks - 3, -1), -1):
        send_own(0, 0, c)
    tok_copy.start()
    w_issue(0, 0)
    w_issue(1, 0)
    for l in range(layers):
        for i in range(3):
            w_own(i, l).start()

    row8 = lax.broadcasted_iota(jnp.int32, (8, ch), 0)
    ogv = og[...].astype(F32)
    acc = jnp.zeros((8, ch), F32)
    for l in range(layers):
        acc = jnp.where(row8 == l, ogv[l : l + 1], acc)
    ogf[my] = acc
    og_copies = [
        pltpu.make_async_remote_copy(
            src_ref=ogf.at[my], dst_ref=ogf.at[my],
            send_sem=og_send.at[d], recv_sem=og_recv.at[my],
            device_id=dev(tp=(my + d) % n_tp),
        )
        for d in range(1, n_tp)
    ]
    for copy in og_copies:
        copy.start()
    heads, head = am.shape[1], am.shape[2]
    for l in range(layers):
        for src, dst in ((am, bda), (im, bdi)):
            for h in range(heads):
                m = src[l, h].astype(F32)
                parts = [m if j == h else jnp.zeros((head, head), F32) for j in range(heads)]
                line = jnp.concatenate(parts, axis=1) if heads > 1 else m
                dst[l, h * head : (h + 1) * head, :] = line.astype(BF16)
    for l in range(layers):
        @pl.when(me == 0)
        def _():
            xp[l, 0:PAD, :] = jnp.zeros((PAD, ch), F32)

    def rim_copy(l):
        return pltpu.make_async_remote_copy(
            src_ref=xp.at[l, pl.ds(tok_rows, PAD)], dst_ref=xp.at[l, pl.ds(0, PAD)],
            send_sem=rim_sem.at[l, 0], recv_sem=rim_sem.at[l, 1],
            device_id=dev(sp=(me + 1) % n_sp),
        )

    def norm(l, c):
        r = rows(c)
        total = jnp.zeros((t_rows, 1), F32)
        for p in range(n_tp):
            v = xs[l, p, r, :].astype(F32)
            total = total + jnp.sum(v * v, axis=1, keepdims=True)
        rs = lax.rsqrt(total / (n_tp * cols) + EPS)
        for p in range(n_tp):
            v = xs[l, p, r, :].astype(F32)
            g = gain[l : l + 1, p * cols : (p + 1) * cols].astype(F32)
            nrm[p, r, :] = (v * rs * g).astype(BF16)

    def project(l, c):
        r = rows(c)
        xr = jnp.zeros((t_rows, ch), F32)
        gr = jnp.zeros((t_rows, ch), F32)
        for p in range(n_tp):
            nv = nrm[p, r, :]
            xr += jnp.dot(nv, wx[l, p * cols : (p + 1) * cols, :], preferred_element_type=F32)
            gr += jnp.dot(nv, wg[l, p * cols : (p + 1) * cols, :], preferred_element_type=F32)
        xp[l, pl.ds(pl.multiple_of(c * t_rows + PAD, 8), t_rows), :] = xr.astype(BF16).astype(F32)
        gl[c] = jax.nn.gelu(gr.astype(BF16).astype(F32))

    def gates(l, c):
        blk = xp[l, pl.ds(pl.multiple_of(c * t_rows, 8), t_rows + PAD), :]
        conv = jnp.zeros((t_rows, ch), F32)
        for j in range(WIDTH):
            o = PAD - (WIDTH - 1) + j
            conv = conv + taps[l, j : j + 1, :].astype(F32) * blk[o : o + t_rows]
        xc = conv.astype(BF16)
        rg = jax.nn.sigmoid(jnp.dot(xc, bda[l], preferred_element_type=F32))
        ig = jax.nn.sigmoid(jnp.dot(xc, bdi[l], preferred_element_type=F32))
        pv = pj[rows(c), :]
        log_a = (-GATE_C * rate[l : l + 1, :]) * rg * pv[:, 0:1] + pv[:, 1:2]
        av = jnp.exp(log_a)
        bv = jnp.sqrt(one_minus_exp(2.0 * log_a)) * ig * xc.astype(F32)
        lw = a_s.shape[3]
        for q in range(a_s.shape[1]):
            a_s[c, q] = av[:, q * lw : (q + 1) * lw]
            b_s[c, q] = bv[:, q * lw : (q + 1) * lw]
            pa = jnp.ones((SEGS, lw), F32)
            hb = jnp.zeros((SEGS, lw), F32)
            for j in range(seg):
                at = pl.ds(j, SEGS, stride=seg)
                x = a_s[c, q, at, :]
                hb = x * hb + b_s[c, q, at, :]
                pa = x * pa
                a_s[c, q, at, :] = pa
                b_s[c, q, at, :] = hb
            ea = jnp.ones((1, lw), F32)
            eb = jnp.zeros((1, lw), F32)
            for s in range(SEGS):
                ea_s[c, q, s : s + 1, :] = ea
                eb_s[c, q, s : s + 1, :] = eb
                eb = pa[s : s + 1] * eb + hb[s : s + 1]
                ea = pa[s : s + 1] * ea
            tot[c, 0:1, q * lw : (q + 1) * lw] = ea
            tot[c, 1:2, q * lw : (q + 1) * lw] = eb

    def st_copy(l, to):
        return pltpu.make_async_remote_copy(
            src_ref=st.at[l, me], dst_ref=st.at[l, me],
            send_sem=st_send.at[l, to], recv_sem=st_recv.at[l, me],
            device_id=dev(sp=to),
        )

    def mix(l, c, inc):
        lw = a_s.shape[3]
        halves = []
        for q in range(a_s.shape[1]):
            part = inc[:, q * lw : (q + 1) * lw]
            lines = []
            for s in range(SEGS):
                entry = eb_s[c, q, s : s + 1, :] + ea_s[c, q, s : s + 1, :] * part
                at = slice(s * seg, (s + 1) * seg)
                lines.append(b_s[c, q, at, :] + a_s[c, q, at, :] * entry)
            halves.append(jnp.concatenate(lines, axis=0))
        state = jnp.concatenate(halves, axis=1) if len(halves) > 1 else halves[0]
        rec = state * gl[c]
        mx[l, my, rows(c), :] = (rec * og[l : l + 1, :].astype(F32)).astype(BF16)

    def update(l, c):
        r = rows(c)
        total = jnp.zeros((t_rows, 1), F32)
        acc = jnp.zeros((t_rows, cols), F32)
        for p in range(n_tp):
            m = mx[l, p, r, :]
            v = m.astype(F32) * (1.0 / ogf[p, l : l + 1, :])
            total = total + jnp.sum(v * v, axis=1, keepdims=True)
            acc += jnp.dot(m, wo[l, p * ch : (p + 1) * ch, :], preferred_element_type=F32)
        scale = lax.rsqrt(total / (n_tp * ch) + EPS)
        new = (xs[l, my, r, :].astype(F32) + acc * scale).astype(BF16)
        if l == layers - 1:
            out[r, :] = new
        else:
            xs[l + 1, my, r, :] = new
            send_own(0, l + 1, c)

    tok_copy.wait()
    for l in range(layers):
        def front(i, carry):
            c = chunks - 1 - i

            near(0, l, c)
            if l == 0:
                @pl.when(c >= 2)
                def _():
                    send_own(0, 0, c - 2)

            @pl.when(i >= 1)
            def _():
                farther(0, l, c + 1)
                norm(l, c + 1)

            return carry

        lax.fori_loop(0, chunks, front, 0)
        w_forward(0, l)
        w_forward(1, l)
        w_issue(2, l)
        w_ready(0, l)
        w_ready(1, l)

        def middle(i, carry):
            c = chunks - 1 - i

            @pl.when(i == chunks - 1)
            def _():
                farther(0, l, 0)
                norm(l, 0)

            project(l, c)

            @pl.when((i == 0) & (me < n_sp - 1))
            def _():
                rim_copy(l).start()

            @pl.when(i >= 1)
            def _():
                gates(l, c + 1)

            return carry

        lax.fori_loop(0, chunks, middle, 0)

        @pl.when(me > 0)
        def _():
            rim_copy(l).wait_recv()

        gates(l, 0)

        ta, tb = jnp.ones((1, ch), F32), jnp.zeros((1, ch), F32)
        for c in range(chunks):
            tb = tot[c, 0:1, :] * tb + tot[c, 1:2, :]
            ta = tot[c, 0:1, :] * ta
        st[l, me] = jnp.where(row8 == 0, ta, tb)

        def send_st(to, carry):
            st_copy(l, to).start()
            return carry

        lax.fori_loop(me + 1, n_sp, send_st, 0)
        w_forward(2, l)
        if l + 1 < layers:
            w_issue(0, l + 1)
            w_issue(1, l + 1)

        def take_st(src, inc):
            place = st.at[l, src]
            pltpu.make_async_copy(place, place, st_recv.at[l, src]).wait()
            return st[l, src, 0:1, :] * inc + st[l, src, 1:2, :]

        inc = lax.fori_loop(0, me, take_st, jnp.zeros((1, ch), F32))
        incs = []
        for c in range(chunks):
            incs.append(inc)
            inc = tot[c, 0:1, :] * inc + tot[c, 1:2, :]
        for c in range(chunks - 1, -1, -1):
            mix(l, c, incs[c])
            if c >= chunks - 2:
                send_own(1, l, c)
        w_ready(2, l)
        if l == 0:
            for d in range(1, n_tp):
                src = (my + d) % n_tp
                pltpu.make_async_copy(ogf.at[src], ogf.at[src], og_recv.at[src]).wait()

        def back(i, carry):
            c = chunks - 1 - i

            @pl.when(i < chunks)
            def _():
                near(1, l, c)

                @pl.when(c >= 2)
                def _():
                    send_own(1, l, c - 2)

            @pl.when(i >= 1)
            def _():
                farther(1, l, c + 1)
                update(l, c + 1)

            return carry

        lax.fori_loop(0, chunks + 1, back, 0)

    def drain(c, carry):
        for kind in range(2):
            for l in range(layers):
                for copy in own_copies(kind, l, c):
                    copy.wait_send()
                if relay:
                    for copy in fwd_copies(kind, l, c):
                        copy.wait_send()
        return carry

    lax.fori_loop(0, chunks, drain, 0)
    for l in range(layers):
        for i in range(3):
            w_wait(i, l, w_send.at[i, l], n_z)
            w_wait(i, l, w_fsend.at[i, l], n_z - 1)

        @pl.when(me < n_sp - 1)
        def _():
            rim_copy(l).wait_send()

        def st_done(to, carry):
            st_copy(l, to).wait_send()
            return carry

        lax.fori_loop(me + 1, n_sp, st_done, 0)
    for copy in og_copies:
        copy.wait_send()


def body(n_sp, n_tp, tokens, mix_gain, x_weight, gate_weight, conv_taps, a_maps, i_maps,
         decay_rate, pace, jumps, out_gain, out_weight):
    layers = x_weight.shape[0]
    tok_rows, cols = tokens.shape
    ch = x_weight.shape[2]
    d = n_tp * cols
    d_rec = n_tp * ch
    chunks = 4
    t_rows = tok_rows // chunks
    lw = min(ch, 128)
    nq = ch // lw
    pj = jnp.stack([pace, jumps], axis=1)
    vm = pl.BlockSpec(memory_space=pltpu.VMEM)
    hb = pl.BlockSpec(memory_space=pl.ANY)
    dma = pltpu.SemaphoreType.DMA
    return pl.pallas_call(
        functools.partial(kernel, (n_sp, n_tp, layers, chunks)),
        out_shape=jax.ShapeDtypeStruct((tok_rows, cols), BF16),
        in_specs=[hb, vm, hb, hb, vm, vm, vm, vm, vm, vm, hb],
        out_specs=vm,
        scratch_shapes=[
            pltpu.VMEM((n_tp, tok_rows, cols), BF16),
            pltpu.VMEM((layers, n_tp, tok_rows, cols), BF16),
            pltpu.VMEM((layers, n_tp, tok_rows, ch), BF16),
            pltpu.VMEM((layers, d, ch), BF16),
            pltpu.VMEM((layers, d, ch), BF16),
            pltpu.VMEM((layers, d_rec, cols), BF16),
            pltpu.VMEM((layers, ch, ch), BF16),
            pltpu.VMEM((layers, ch, ch), BF16),
            pltpu.VMEM((layers, PAD + tok_rows, ch), F32),
            pltpu.VMEM((chunks, t_rows, ch), F32),
            pltpu.VMEM((chunks, nq, t_rows, lw), F32),
            pltpu.VMEM((chunks, nq, t_rows, lw), F32),
            pltpu.VMEM((chunks, nq, SEGS, lw), F32),
            pltpu.VMEM((chunks, nq, SEGS, lw), F32),
            pltpu.VMEM((chunks, 8, ch), F32),
            pltpu.VMEM((layers, n_sp, 8, ch), F32),
            pltpu.VMEM((n_tp, 8, ch), F32),
            dma((2, layers, chunks, n_tp)),
            dma((2, layers, chunks, n_tp)),
            dma((3, layers)),
            dma((3, layers)),
            dma((3, layers)),
            dma((3, layers)),
            dma((3, layers)),
            dma,
            dma((layers, 2)),
            dma((layers, n_sp)),
            dma((layers, n_sp)),
            dma((n_tp,)),
            dma((n_tp,)),
        ],
        compiler_params=pltpu.CompilerParams(
            collective_id=0, has_side_effects=True, vmem_limit_bytes=60 * 1024 * 1024
        ),
    )(tokens, mix_gain, x_weight, gate_weight, conv_taps, a_maps, i_maps, decay_rate, pj,
      out_gain, out_weight)


def solution(mesh):
    in_specs = (
        P("sp", "tp"),
        P(),
        P(None, "sp", "tp"),
        P(None, "sp", "tp"),
        P(None, None, "tp"),
        P(None, "tp", None, None),
        P(None, "tp", None, None),
        P(None, "tp"),
        P("sp"),
        P("sp"),
        P(None, "tp"),
        P(None, "sp", "tp"),
    )
    out_specs = P("sp", "tp")
    return jax.shard_map(
        functools.partial(body, mesh.shape["sp"], mesh.shape["tp"]),
        mesh=mesh, in_specs=in_specs, out_specs=out_specs, check_vma=False,
    )
```
